32 devices in a mesh: fs: 8 (over z, x), tp: 4 (over y, core).
Axes of the slice: x: 2, y: 2, z: 4, core: 2. Of those that a mesh axis runs over, the one named last changes fastest.
Arguments:
- tokens: bfloat16 [4096, 2048], P(('fs', 'tp')), may hold values from -6 to 6
- norm_gain: float32 [2048], replicated, may hold values from 0.1 to 1.9
- up_weight: bfloat16 [2048, 8192], P('fs', 'tp'), may hold values from -0.125 to 0.125
- down_weight: bfloat16 [8192, 2048], P('tp', 'fs'), may hold values from -0.0625 to 0.0625
Outputs:
- mixed: bfloat16 [4096, 2048], P(('fs', 'tp'))
The draws below stay inside these ranges and needn't reach their ends.
All inputs are finite; a program needn't handle non-finite values.
Results may differ from the reference program's by a relative error of at most 0.013.
Values may be sent and summed in bfloat16 or wider, within the bound.
No kernel may reach another device: no remote copies, remote signals or barrier semaphores. Data moves between devices by JAX's collectives and lax.ppermute only.
A program may use at most 64 MiB of HBM per device.

```python
import jax
import jax.numpy as jnp
from jax import lax

D = 2048
FF = 8192
TOKENS = 4096
N_TP = 4


def level_of(own_key, extent, shards, low, largest):
    loudness, own = 1.0, jax.random.fold_in(own_key, 6)
    for axis_at, parts in shards:
        heights = jnp.exp(jax.random.uniform(jax.random.fold_in(own, axis_at), (parts,), jnp.float32, low / len(shards), largest / len(shards)))
        loudness = loudness * jnp.repeat(heights, extent[axis_at] // parts).reshape([-1 if axis == axis_at else 1 for axis in range(len(extent))])
    return loudness


def normal_values(own_key, extent, deviation, reach, split=(), held_as=jnp.bfloat16):
    array = jax.random.normal(own_key, extent, jnp.float32) * deviation
    if len(split) > 0:
        array = level_of(own_key, extent, split, -0.22, 0.18) * array
    return jnp.clip(array, min=-reach, max=reach).astype(held_as)


def setup_inputs(seed: int = 0) -> dict:
    streams_of = jax.random.split(jax.random.key(seed), 5)
    return {
        "tokens": normal_values(streams_of[0], (TOKENS, D), 1.0, 6.0, ((0, 32),)),
        "norm_gain": jnp.clip(1.0 + 0.18 * jax.random.normal(streams_of[1], (D,), jnp.float32), 0.1, 1.9),
        "up_weight": normal_values(streams_of[2], (D, FF), D ** -0.5, 0.125, ((0, 8), (1, 4))),
        "down_weight": normal_values(streams_of[3], (FF, D), FF ** -0.5, 0.0625, ((0, 4), (1, 8))),
    }


epsilon = 1e-06

def reference(tokens, norm_gain, up_weight, down_weight):
    values = tokens.astype(jnp.float32)
    mean_square = lax.optimization_barrier(jnp.mean(values * values, axis=-1, keepdims=True))
    normed = (values * lax.rsqrt(mean_square + epsilon) * norm_gain).astype(jnp.bfloat16)
    preact = jnp.dot(normed, up_weight, preferred_element_type=jnp.float32)
    hidden = jnp.square(jnp.maximum(preact, 0.0)).astype(jnp.bfloat16)
    width = FF // N_TP
    total = jnp.zeros((tokens.shape[0], D), jnp.float32)
    for block in range(N_TP):
        columns = hidden[:, block * width:(block + 1) * width]
        rows_down = down_weight[block * width:(block + 1) * width, :]
        partial_value = jnp.dot(columns, rows_down, preferred_element_type=jnp.float32).astype(jnp.bfloat16)
        partial_value = lax.optimization_barrier(partial_value)
        total = total + partial_value.astype(jnp.float32)
    return total.astype(jnp.bfloat16)
```

```python
import jax
import jax.numpy as jnp
from jax import lax
from jax.sharding import Mesh, PartitionSpec as P

epsilon = 1e-06


def squared_relu(preact):
    return jnp.square(jnp.maximum(preact, 0.0)).astype(jnp.bfloat16)


def shifted(value, axis, size, step):
    return lax.ppermute(value, axis, [(i, (i + step) % size) for i in range(size)])


def exchange(piece_for, axis, size, like):
    own = lax.axis_index(axis)
    out = jnp.zeros((size,) + like.shape, like.dtype)
    out = lax.dynamic_update_index_in_dim(out, piece_for(own), own, 0)
    for step in range(1, size):
        got = shifted(piece_for((own + step) % size), axis, size, step)
        out = lax.dynamic_update_index_in_dim(out, got, (own - step) % size, 0)
    return out


def solution(mesh):
    fs, tp = mesh.shape["fs"], mesh.shape["tp"]
    n_x = 1
    while (2 * n_x) ** 2 <= fs:
        n_x *= 2
    n_z, n_c = fs // n_x, 2
    n_y = tp // n_c
    split = Mesh(mesh.devices.reshape(n_z, n_x, n_y, n_c), ("z", "x", "y", "c"))

    def on_device(tokens, norm_gain, up_weight, down_weight):
        values = tokens.astype(jnp.float32)
        mean_square = jnp.mean(values * values, axis=-1, keepdims=True)
        normed = (values * lax.rsqrt(mean_square + epsilon) * norm_gain).astype(jnp.bfloat16)
        rows, width = up_weight.shape
        part = width // n_z

        up_piece = lambda z: lax.dynamic_slice_in_dim(up_weight, z * part, part, 1)
        down_piece = lambda z: lax.dynamic_slice_in_dim(down_weight, z * part, part, 0)
        up = exchange(up_piece, "z", n_z, jax.ShapeDtypeStruct((rows, part), up_weight.dtype))
        down = exchange(down_piece, "z", n_z, jax.ShapeDtypeStruct((part, rows), down_weight.dtype))
        up = exchange(lambda x: up, "x", n_x, up)
        down = exchange(lambda x: down, "x", n_x, down)
        up = up.transpose(1, 0, 2, 3).reshape(fs * rows, part)
        down = down.transpose(2, 1, 0, 3).reshape(part, fs * rows)
        up_other = shifted(up, "c", n_c, 1)
        down_other = shifted(down, "c", n_c, 1)

        whole = lax.all_gather(normed, ("z", "y"), axis=0, tiled=True)
        hidden = [
            squared_relu(jnp.dot(whole, w, preferred_element_type=jnp.float32))
            for w in (up, up_other)
        ]
        partial_value = jnp.dot(
            jnp.concatenate(hidden, axis=1),
            jnp.concatenate([down, down_other], axis=0),
            preferred_element_type=jnp.float32,
        ).astype(jnp.bfloat16)
        return lax.psum_scatter(partial_value, ("z", "y"), scatter_dimension=0, tiled=True)

    tokens_at = P(("z", "x", "y", "c"), None)
    placed = (tokens_at, P(), P(("z", "x"), ("y", "c")), P(("y", "c"), ("z", "x")))
    return jax.shard_map(
        on_device, mesh=split, in_specs=placed, out_specs=tokens_at, check_vma=False
    )
```

```python
import jax
import jax.numpy as jnp
from jax import lax
from jax.sharding import Mesh, PartitionSpec as P

epsilon = 1e-06


def squared_relu(preact):
    return jnp.square(jnp.maximum(preact, 0.0)).astype(jnp.bfloat16)


def solution(mesh):
    fs, tp = mesh.shape["fs"], mesh.shape["tp"]
    n_x = 1
    while (2 * n_x) ** 2 <= fs:
        n_x *= 2
    n_z, n_c = fs // n_x, 2
    n_y, n_h = tp // n_c, n_z // n_c
    split = Mesh(
        mesh.devices.reshape(n_h, n_c, n_x, n_y, n_c), ("h", "l", "x", "y", "c")
    )

    def collect(block):
        h, x, c = (lax.axis_index(axis) for axis in "hxc")
        for step in range(n_h):
            pairs = []
            for z in range(n_z):
                for core in range(n_c):
                    to = ((z + step) % n_h) * n_c + core
                    pairs.append((z * n_c + core, to * n_c + z // n_h))
            own = lax.ppermute(block, ("h", "l", "c"), pairs)
            z_low = (h - step) % n_h
            for hop in range(n_x):
                got = own
                if hop:
                    got = lax.ppermute(
                        own, "x", [(i, (i + hop) % n_x) for i in range(n_x)]
                    )
                from_x = (x - hop) % n_x
                yield (c * n_h + z_low) * n_x + from_x, got
                other = lax.ppermute(got, "c", [(0, 1), (1, 0)])
                yield ((1 - c) * n_h + z_low) * n_x + from_x, other

    def on_device(tokens, norm_gain, up_weight, down_weight):
        values = tokens.astype(jnp.float32)
        mean_square = jnp.mean(values * values, axis=-1, keepdims=True)
        normed = (values * lax.rsqrt(mean_square + epsilon) * norm_gain).astype(jnp.bfloat16)
        rows, width = up_weight.shape
        whole = lax.all_gather(normed, ("l", "y"), axis=0, tiled=True)

        up_pieces = list(collect(up_weight))
        down_pieces = list(collect(down_weight))
        up = jnp.zeros((fs * rows, width), up_weight.dtype)
        for at, piece in up_pieces:
            up = lax.dynamic_update_slice_in_dim(up, piece, at * rows, 0)
        hidden = squared_relu(jnp.dot(whole, up, preferred_element_type=jnp.float32))
        partial_value = jnp.zeros(whole.shape, jnp.bfloat16)
        for at, piece in down_pieces:
            made = jnp.dot(hidden, piece, preferred_element_type=jnp.float32)
            partial_value = lax.dynamic_update_slice_in_dim(
                partial_value, made.astype(jnp.bfloat16), at * rows, 1
            )
        return lax.psum_scatter(partial_value, ("l", "y"), scatter_dimension=0, tiled=True)

    tokens_at = P(("h", "l", "x", "y", "c"), None)
    placed = (
        tokens_at,
        P(),
        P(("h", "l", "x"), ("y", "c")),
        P(("y", "c"), ("h", "l", "x")),
    )
    return jax.shard_map(
        on_device, mesh=split, in_specs=placed, out_specs=tokens_at, check_vma=False
    )
```

```python
import jax
import jax.numpy as jnp
from jax import lax
from jax.sharding import Mesh, PartitionSpec as P

epsilon = 1e-06


def squared_relu(preact):
    return jnp.square(jnp.maximum(preact, 0.0)).astype(jnp.bfloat16)


def solution(mesh):
    fs, tp = mesh.shape["fs"], mesh.shape["tp"]
    n_x = 1
    while (2 * n_x) ** 2 <= fs:
        n_x *= 2
    n_z, n_c = fs // n_x, 2
    n_y, n_h = tp // n_c, n_z // n_c
    split = Mesh(
        mesh.devices.reshape(n_h, n_c, n_x, n_y, n_c), ("h", "l", "x", "y", "c")
    )

    def collect(block):
        h, x, c = (lax.axis_index(axis) for axis in "hxc")
        for step in range(n_h):
            pairs = []
            for z in range(n_z):
                for core in range(n_c):
                    to = ((z + step) % n_h) * n_c + core
                    pairs.append((z * n_c + core, to * n_c + z // n_h))
            own = lax.ppermute(block, ("h", "l", "c"), pairs)
            z_low = (h - step) % n_h
            for hop in range(n_x):
                got = own
                if hop:
                    got = lax.ppermute(
                        own, "x", [(i, (i + hop) % n_x) for i in range(n_x)]
                    )
                from_x = (x - hop) % n_x
                yield (c * n_h + z_low) * n_x + from_x, got
                other = lax.ppermute(got, "c", [(0, 1), (1, 0)])
                yield ((1 - c) * n_h + z_low) * n_x + from_x, other

    peers = [(l, y) for l in range(n_c) for y in range(n_y)]

    def to_peer(value, l_step, y_step):
        pairs = [
            (l * n_y + y, (l + l_step) % n_c * n_y + (y + y_step) % n_y) for l, y in peers
        ]
        return lax.ppermute(value, ("l", "y"), pairs)

    def on_device(tokens, norm_gain, up_weight, down_weight):
        values = tokens.astype(jnp.float32)
        mean_square = jnp.mean(values * values, axis=-1, keepdims=True)
        normed = (values * lax.rsqrt(mean_square + epsilon) * norm_gain).astype(jnp.bfloat16)
        count = normed.shape[0]
        rows, width = up_weight.shape
        whole = jnp.concatenate(
            [normed] + [to_peer(normed, l, y) for l, y in peers[1:]], axis=0
        )

        up_pieces = list(collect(up_weight))
        down_pieces = list(collect(down_weight))
        up = jnp.zeros((fs * rows, width), up_weight.dtype)
        for at, piece in up_pieces:
            up = lax.dynamic_update_slice_in_dim(up, piece, at * rows, 0)
        hidden = squared_relu(jnp.dot(whole, up, preferred_element_type=jnp.float32))
        group = len(down_pieces) // n_h
        mixed = jnp.zeros(tokens.shape, jnp.bfloat16)
        for step in range(n_h):
            chosen = down_pieces[step * group:(step + 1) * group]
            made = jnp.concatenate(
                [
                    jnp.dot(hidden, piece, preferred_element_type=jnp.float32).astype(
                        jnp.bfloat16
                    )
                    for _, piece in chosen
                ],
                axis=1,
            )
            total = made[:count].astype(jnp.float32)
            for p, (l, y) in list(enumerate(peers))[:0:-1]:
                got = to_peer(made[p * count:(p + 1) * count], -l, -y)
                total = total + got.astype(jnp.float32)
            total = total.astype(jnp.bfloat16)
            for i, (at, _) in enumerate(chosen):
                mixed = lax.dynamic_update_slice_in_dim(
                    mixed, total[:, i * rows:(i + 1) * rows], at * rows, 1
                )
        return mixed

    tokens_at = P(("h", "l", "x", "y", "c"), None)
    placed = (
        tokens_at,
        P(),
        P(("h", "l", "x"), ("y", "c")),
        P(("y", "c"), ("h", "l", "x")),
    )
    return jax.shard_map(
        on_device, mesh=split, in_specs=placed, out_specs=tokens_at, check_vma=False
    )
```

```python
import jax
import jax.numpy as jnp
from jax import lax
from jax.sharding import Mesh, PartitionSpec as P

epsilon = 1e-06


def squared_relu(preact):
    return jnp.square(jnp.maximum(preact, 0.0)).astype(jnp.bfloat16)


def solution(mesh):
    fs, tp = mesh.shape["fs"], mesh.shape["tp"]
    n_x = 1
    while (2 * n_x) ** 2 <= fs:
        n_x *= 2
    n_z, n_c = fs // n_x, 2
    n_y, n_h = tp // n_c, n_z // n_c
    split = Mesh(
        mesh.devices.reshape(n_h, n_c, n_x, n_y, n_c), ("h", "l", "x", "y", "c")
    )

    def collect(block):
        h, x, c = (lax.axis_index(axis) for axis in "hxc")
        places, held = [], []
        for step in range(n_h):
            pairs = []
            for z in range(n_z):
                for core in range(n_c):
                    to = ((z + step) % n_h) * n_c + core
                    pairs.append((z * n_c + core, to * n_c + z // n_h))
            own = lax.ppermute(block, ("h", "l", "c"), pairs)
            for hop in range(n_x):
                got = own
                if hop:
                    got = lax.ppermute(
                        own, "x", [(i, (i + hop) % n_x) for i in range(n_x)]
                    )
                places.append(((h - step) % n_h, (x - hop) % n_x))
                held.append(got)
        held = lax.optimization_barrier(held)
        pieces = []
        for (z_low, from_x), got in zip(places, held):
            other = lax.ppermute(got, "c", [(0, 1), (1, 0)])
            pieces.append(((c * n_h + z_low) * n_x + from_x, got))
            pieces.append((((1 - c) * n_h + z_low) * n_x + from_x, other))
        return pieces

    peers = [(l, y) for l in range(n_c) for y in range(n_y)]

    def to_peer(value, l_step, y_step):
        pairs = [
            (l * n_y + y, (l + l_step) % n_c * n_y + (y + y_step) % n_y) for l, y in peers
        ]
        return lax.ppermute(value, ("l", "y"), pairs)

    def on_device(tokens, norm_gain, up_weight, down_weight):
        values = tokens.astype(jnp.float32)
        mean_square = jnp.mean(values * values, axis=-1, keepdims=True)
        normed = (values * lax.rsqrt(mean_square + epsilon) * norm_gain).astype(jnp.bfloat16)
        normed, up_weight, down_weight = lax.optimization_barrier(
            (normed, up_weight, down_weight)
        )
        count = normed.shape[0]
        rows, width = up_weight.shape
        whole = jnp.concatenate(
            [normed] + [to_peer(normed, l, y) for l, y in peers[1:]], axis=0
        )

        up_pieces = collect(up_weight)
        down_pieces = collect(down_weight)
        up = jnp.zeros((fs * rows, width), up_weight.dtype)
        for at, piece in up_pieces:
            up = lax.dynamic_update_slice_in_dim(up, piece, at * rows, 0)
        hidden = squared_relu(jnp.dot(whole, up, preferred_element_type=jnp.float32))
        group = len(down_pieces) // n_h
        mixed = jnp.zeros(tokens.shape, jnp.bfloat16)
        for step in range(n_h):
            chosen = down_pieces[step * group:(step + 1) * group]
            made = jnp.concatenate(
                [
                    jnp.dot(hidden, piece, preferred_element_type=jnp.float32).astype(
                        jnp.bfloat16
                    )
                    for _, piece in chosen
                ],
                axis=1,
            )
            total = made[:count].astype(jnp.float32)
            for p, (l, y) in list(enumerate(peers))[:0:-1]:
                got = to_peer(made[p * count:(p + 1) * count], -l, -y)
                total = total + got.astype(jnp.float32)
            total = total.astype(jnp.bfloat16)
            for i, (at, _) in enumerate(chosen):
                mixed = lax.dynamic_update_slice_in_dim(
                    mixed, total[:, i * rows:(i + 1) * rows], at * rows, 1
                )
        return mixed

    tokens_at = P(("h", "l", "x", "y", "c"), None)
    placed = (
        tokens_at,
        P(),
        P(("h", "l", "x"), ("y", "c")),
        P(("y", "c"), ("h", "l", "x")),
    )
    return jax.shard_map(
        on_device, mesh=split, in_specs=placed, out_specs=tokens_at, check_vma=False
    )
```
